32 devices in a mesh: fs: 8 (over z, y), tp: 4 (over x, core).
Axes of the slice: x: 2, y: 2, z: 4, core: 2. Of those that a mesh axis runs over, the one named last changes fastest.
Arguments:
- tokens: bfloat16 [2048, 2048], P('fs', 'tp'), may hold values from -12.1 to 12.1, as said below
- gate_weight: float32 [2048, 5632], P('fs', 'tp'), may hold values from -0.125 to 0.125
- up_weight: float32 [2048, 5632], P('fs', 'tp'), may hold values from -0.125 to 0.125
- down_weight: float32 [5632, 2048], P('tp', 'fs'), may hold values from -0.078125 to 0.078125
- gate_scale: float32 [4, 1408], P('tp', 'fs'), may hold values from 0.1 to 1.9
- up_scale: float32 [4, 1408], P('tp', 'fs'), may hold values from 0.1 to 1.9
- down_scale: float32 [4, 512], P('tp', 'fs'), may hold values from 0.16 to 4.6, as said below
- bgate_weight: float32 [2048, 2048], P('fs', 'tp'), may hold values from -0.125 to 0.125
- cgate_weight: float32 [2048, 2048], P('fs', 'tp'), may hold values from -0.125 to 0.125
- value_weight: float32 [2048, 2048], P('fs', 'tp'), may hold values from -0.125 to 0.125
- bgate_scale: float32 [4, 512], P('tp', 'fs'), may hold values from 0.1 to 1.9
- cgate_scale: float32 [4, 512], P('tp', 'fs'), may hold values from 0.1 to 1.9
- value_scale: float32 [4, 512], P('tp', 'fs'), may hold values from 0.1 to 1.9
- conv_taps: float32 [3, 2048], replicated, may hold values from -3.5 to 3.5
- mixout_weight: float32 [2048, 2048], P('tp', 'fs'), may hold values from -0.125 to 0.125
- mixout_scale: float32 [4, 512], P('tp', 'fs'), may hold values from 0.16 to 4.6, as said below
- first_gain: float32 [2048], replicated, may hold values from 0.1 to 1.9
- first_shift: float32 [2048], replicated, may hold values from -1.8 to 1.8
- mixer_gain: float32 [2048], replicated, may hold values from 0.1 to 1.9
- mixer_shift: float32 [2048], replicated, may hold values from -1.8 to 1.8
- last_gain: float32 [2048], replicated, may hold values from 0.1 to 1.9
- last_shift: float32 [2048], replicated, may hold values from -1.8 to 1.8
Outputs:
- layer_out: bfloat16 [2048, 2048], P('fs', 'tp')
The draws below stay inside these ranges and needn't reach their ends.
Inputs may be any that keep to these rules, and one draw needn't show every extreme that they name: `tokens`: normal values times one factor for each of 4 equal consecutive blocks of the features. `down_scale`: positive; one factor for each row times a spread over the columns. `mixout_scale`: positive; one factor for each row times a spread over the columns.
All inputs are finite; a program needn't handle non-finite values.
Results may differ from the reference program's by a relative error of at most 0.025.
Values may be sent and summed in bfloat16 or wider, within the bound.
A program may use at most 64 MiB of HBM per device.

```python
import jax
import jax.numpy as jnp
from jax import lax

D = 2048
FF = 5632
CONV_CH = 2048
TAPS = 3
LENGTH = 128
TOKENS = 2048
N_TP = 4


def block_factors(key, blocks):
    return jnp.exp(jax.random.uniform(key, (blocks, 1), jnp.float32, -1.1, 1.1))


def draw_tokens(key, part):
    values = jnp.clip(jax.random.normal(jax.random.fold_in(key, 11), (TOKENS, D), jnp.float32), -4.0, 4.0)
    factor = block_factors(jax.random.fold_in(key, 12), N_TP)
    column_factor = jnp.repeat(factor[:, 0], D // N_TP)
    return (values * column_factor[None, :]).astype(jnp.bfloat16)


def column_scale(key):
    factor = block_factors(jax.random.fold_in(key, 1), N_TP)
    spread_part = jax.random.uniform(jax.random.fold_in(key, 2), (N_TP, D // N_TP), jnp.float32, 0.7, 1.3)
    return factor * spread_part


def draw_down_scale(key, part):
    return column_scale(jax.random.fold_in(key, 21))


def draw_mixout_scale(key, part):
    return column_scale(jax.random.fold_in(key, 22))


def block_levels(stream_key, dims, split, smallest, high):
    factor_of, own = 1.0, jax.random.fold_in(stream_key, 6)
    for axis_at, blocks in split:
        draws = jnp.exp(jax.random.uniform(jax.random.fold_in(own, axis_at), (blocks,), jnp.float32, smallest / len(split), high / len(split)))
        factor_of = factor_of * jnp.repeat(draws, dims[axis_at] // blocks).reshape([-1 if axis == axis_at else 1 for axis in range(len(dims))])
    return factor_of


def scatter_about(key, shape, scale, bound, cuts=(), held_as=jnp.bfloat16):
    values = scale * jax.random.normal(key, shape, jnp.float32)
    if cuts:
        values = values * block_levels(key, shape, cuts, -0.22, 0.18)
    return jnp.clip(values, -bound, bound).astype(held_as)


def setup_inputs(seed: int = 0) -> dict:
    key_list = jax.random.split(jax.random.key(seed), 23)
    return {
        "tokens": draw_tokens(jax.random.fold_in(key_list[22], 71), 0),
        "gate_weight": scatter_about(key_list[1], (D, FF), D ** -0.5, 0.125, ((0, 8), (1, 4)), jnp.float32),
        "up_weight": scatter_about(key_list[2], (D, FF), D ** -0.5, 0.125, ((0, 8), (1, 4)), jnp.float32),
        "down_weight": scatter_about(key_list[3], (FF, D), FF ** -0.5, 0.078125, ((0, 4), (1, 8)), jnp.float32),
        "gate_scale": jnp.clip(1.0 + 0.18 * jax.random.normal(key_list[4], (N_TP, FF // N_TP), jnp.float32), 0.1, 1.9),
        "up_scale": jnp.clip(1.0 + 0.18 * jax.random.normal(key_list[5], (N_TP, FF // N_TP), jnp.float32), 0.1, 1.9),
        "down_scale": draw_down_scale(jax.random.fold_in(key_list[22], 71), 0),
        "bgate_weight": scatter_about(key_list[7], (D, CONV_CH), D ** -0.5, 0.125, ((0, 8), (1, 4)), jnp.float32),
        "cgate_weight": scatter_about(key_list[8], (D, CONV_CH), D ** -0.5, 0.125, ((0, 8), (1, 4)), jnp.float32),
        "value_weight": scatter_about(key_list[9], (D, CONV_CH), D ** -0.5, 0.125, ((0, 8), (1, 4)), jnp.float32),
        "bgate_scale": jnp.clip(1.0 + 0.18 * jax.random.normal(key_list[10], (N_TP, CONV_CH // N_TP), jnp.float32), 0.1, 1.9),
        "cgate_scale": jnp.clip(1.0 + 0.18 * jax.random.normal(key_list[11], (N_TP, CONV_CH // N_TP), jnp.float32), 0.1, 1.9),
        "value_scale": jnp.clip(1.0 + 0.18 * jax.random.normal(key_list[12], (N_TP, CONV_CH // N_TP), jnp.float32), 0.1, 1.9),
        "conv_taps": scatter_about(key_list[13], (TAPS, CONV_CH), TAPS ** -0.5, 3.5, (), jnp.float32),
        "mixout_weight": scatter_about(key_list[14], (CONV_CH, D), CONV_CH ** -0.5, 0.125, ((0, 4), (1, 8)), jnp.float32),
        "mixout_scale": draw_mixout_scale(jax.random.fold_in(key_list[22], 71), 0),
        "first_gain": jnp.clip(1.0 + 0.18 * jax.random.normal(key_list[16], (D,), jnp.float32), 0.1, 1.9),
        "first_shift": scatter_about(key_list[17], (D,), 0.3, 1.8, (), jnp.float32),
        "mixer_gain": jnp.clip(1.0 + 0.18 * jax.random.normal(key_list[18], (D,), jnp.float32), 0.1, 1.9),
        "mixer_shift": scatter_about(key_list[19], (D,), 0.3, 1.8, (), jnp.float32),
        "last_gain": jnp.clip(1.0 + 0.18 * jax.random.normal(key_list[20], (D,), jnp.float32), 0.1, 1.9),
        "last_shift": scatter_about(key_list[21], (D,), 0.3, 1.8, (), jnp.float32),
    }


RESIDUAL_SCALE = 1.4142135623730951
HALF_STEP = 0.5
EPSILON = 1e-05

def post_norm(residual, branch, norm_gain, norm_shift):
    summed = RESIDUAL_SCALE * residual.astype(jnp.float32) + branch
    average = lax.optimization_barrier(jnp.mean(summed, -1, keepdims=True))
    mean_square = lax.optimization_barrier(jnp.mean(summed * summed, -1, keepdims=True))
    variance = mean_square - average * average
    return ((summed - average) * lax.rsqrt(variance + EPSILON) * norm_gain + norm_shift).astype(jnp.bfloat16)

def block_sum(left_rows, right_cols):
    block_width = left_rows.shape[1] // N_TP
    running = jnp.zeros((left_rows.shape[0], right_cols.shape[1]), jnp.float32)
    for block_index in range(N_TP):
        low = block_index * block_width
        partial_value = jnp.dot(left_rows[:, low:low + block_width], right_cols[low:low + block_width], preferred_element_type=jnp.float32)
        running = running + lax.optimization_barrier(partial_value.astype(jnp.bfloat16)).astype(jnp.float32)
    return running

def scaled_dot(inputs, matrix, scales):
    product = jnp.dot(inputs, matrix.astype(jnp.bfloat16), preferred_element_type=jnp.float32)
    return product * scales.reshape(-1)

def feed(inputs, gate_weight, up_weight, down_weight, gate_scale, up_scale, down_scale):
    gate_sum = scaled_dot(inputs, gate_weight, gate_scale)
    up_sum = scaled_dot(inputs, up_weight, up_scale)
    hidden = (jax.nn.silu(gate_sum) * up_sum).astype(jnp.bfloat16)
    result = block_sum(hidden, down_weight.astype(jnp.bfloat16)) * down_scale.reshape(-1)
    return HALF_STEP * result

def causal_conv(mixed, conv_taps):
    channels = mixed.shape[1]
    shaped = mixed.reshape(-1, LENGTH, channels)
    padded = jnp.pad(shaped, ((0, 0), (TAPS - 1, 0), (0, 0)))
    convolved = jnp.zeros(shaped.shape, jnp.float32)
    for tap_index in range(TAPS):
        convolved = convolved + conv_taps[tap_index] * padded[:, tap_index:tap_index + LENGTH]
    return convolved.reshape(-1, channels)

def reference(tokens, gate_weight, up_weight, down_weight, gate_scale, up_scale, down_scale, bgate_weight, cgate_weight, value_weight, bgate_scale, cgate_scale, value_scale, conv_taps, mixout_weight, mixout_scale, first_gain, first_shift, mixer_gain, mixer_shift, last_gain, last_shift):
    ffn_args = (gate_weight, up_weight, down_weight, gate_scale, up_scale, down_scale)
    first = post_norm(tokens, feed(tokens, *ffn_args), first_gain, first_shift)
    outgate = scaled_dot(first, bgate_weight, bgate_scale)
    ingate = scaled_dot(first, cgate_weight, cgate_scale)
    values = scaled_dot(first, value_weight, value_scale)
    convolved = causal_conv(ingate * values, conv_taps)
    gated = (outgate * convolved).astype(jnp.bfloat16)
    token_mix = block_sum(gated, mixout_weight.astype(jnp.bfloat16)) * mixout_scale.reshape(-1)
    second = post_norm(first, token_mix, mixer_gain, mixer_shift)
    return post_norm(second, feed(second, *ffn_args), last_gain, last_shift)
```

```python
import functools

import jax
import jax.numpy as jnp
from jax import lax
from jax.experimental import pallas as pl
from jax.experimental.pallas import tpu as pltpu
from jax.sharding import Mesh
from jax.sharding import PartitionSpec as P

TAPS = 3
LENGTH = 128
CORES = 2

RESIDUAL_SCALE = 1.4142135623730951
HALF_STEP = 0.5
EPSILON = 1e-05
BY_AXIS = pl.DeviceIdType.MESH
ANY = pl.BlockSpec(memory_space=pl.ANY)
VMEM = pl.BlockSpec(memory_space=pltpu.VMEM)


def greet(depth, axes):
    barrier = pltpu.get_barrier_semaphore()
    z = lax.axis_index("z")
    targets = [{"z": lax.rem(z + d, depth)} for d in range(1, depth)]
    targets += [{axis: 1 - lax.axis_index(axis)} for axis in axes]
    for target in targets:
        pl.semaphore_signal(barrier, inc=1, device_id=target, device_id_type=BY_AXIS)
    pl.semaphore_wait(barrier, len(targets))


def remote(src, dst, send, recv, target):
    return pltpu.make_async_remote_copy(
        src_ref=src, dst_ref=dst, send_sem=send, recv_sem=recv, device_id=target, device_id_type=BY_AXIS
    )


def start_gather(depth, own, whole, z, c, sems):
    zsend, zrecv, csend, crecv, local = sems
    keep = pltpu.make_async_copy(own, whole.at[z, c], local)
    keep.start()
    across = []
    for d in range(1, depth):
        copy = remote(own, whole.at[z, c], zsend.at[d], zrecv.at[d], {"z": lax.rem(z + d, depth)})
        copy.start()
        across.append(copy)
    beside = [remote(own, whole.at[z, c], csend.at[0], crecv.at[0], {"c": 1 - c})]
    beside[0].start()
    return keep, across, beside


def end_gather(depth, whole, z, c, sems, state):
    zsend, zrecv, csend, crecv, local = sems
    keep, across, beside = state
    for d in range(1, depth):
        across[d - 1].wait_recv()
        place = whole.at[lax.rem(z - d + depth, depth), c]
        copy = remote(place, place, csend.at[d], crecv.at[d], {"c": 1 - c})
        copy.start()
        beside.append(copy)
    for copy in beside:
        copy.wait()
    for copy in across:
        copy.wait_send()
    keep.wait()


def weights_kernel(
    depth, w_ref, s_ref, t_ref, g_ref, sa_ref, ta_ref,
    zsend, zrecv, ysend, yrecv, xsend, xrecv, dsend, drecv,
    ssend, srecv, tzsend, tzrecv, tcsend, tcrecv, local,
):
    z, y, x, c = (lax.axis_index(axis) for axis in ("z", "y", "x", "c"))
    width = w_ref.shape[2]
    greet(depth, ("y", "x", "c"))

    def place(px, pz, py):
        start = pl.multiple_of((pz * 2 + py) * width, width)
        return g_ref.at[px, :, pl.ds(start, width)]

    to_x, to_y, to_c = {"x": 1 - x}, {"y": 1 - y}, {"c": 1 - c}
    own_scale = pltpu.make_async_copy(s_ref, sa_ref.at[c, x, y, z], local.at[0])
    own_scale.start()
    scale_sends = []
    for d in range(1, depth):
        copy = remote(s_ref, sa_ref.at[c, x, y, z], ssend.at[d], srecv.at[d], {"z": lax.rem(z + d, depth)})
        copy.start()
        scale_sends.append(copy)
    token_sems = (tzsend, tzrecv, tcsend, tcrecv, local.at[1])
    token_state = start_gather(depth, t_ref, ta_ref, z, c, token_sems)
    z_copies = []
    for d in range(1, depth):
        target = lax.rem(z + d, depth)
        copy = remote(w_ref.at[target], place(x, z, y), zsend.at[d], zrecv.at[d], {"z": target})
        copy.start()
        z_copies.append(copy)
    keep = pltpu.make_async_copy(w_ref.at[z], place(x, z, y), local.at[2])
    keep.start()

    y_copies, x_copies, d_copies = [], [], []

    def relay(d):
        source = lax.rem(z - d + depth, depth)
        if d % 2 == 0:
            y_copies[d].wait_recv()
            block = place(x, source, 1 - y)
            copy = remote(block, block, dsend.at[d], drecv.at[d], to_x)
        else:
            x_copies[d].wait_recv()
            block = place(1 - x, source, y)
            copy = remote(block, block, dsend.at[d], drecv.at[d], to_y)
        copy.start()
        d_copies.append(copy)

    for d in range(depth):
        source = lax.rem(z - d + depth, depth)
        block = place(x, source, y)
        origin = w_ref.at[z] if d == 0 else block
        if d > 0:
            z_copies[d - 1].wait_recv()
        ycopy = remote(origin, block, ysend.at[d], yrecv.at[d], to_y)
        xcopy = remote(origin, block, xsend.at[d], xrecv.at[d], to_x)
        ycopy.start()
        xcopy.start()
        y_copies.append(ycopy)
        x_copies.append(xcopy)
        if d > 0:
            relay(d - 1)
        if d == 0:
            own_scale.wait()
            for copy in scale_sends:
                copy.wait()
            column = sa_ref.at[c, x, y]
            hop = remote(column, column, ssend.at[0], srecv.at[0], to_y)
            hop.start()
            hop.wait()
            plane = sa_ref.at[c, x]
            hop = remote(plane, plane, ssend.at[depth], srecv.at[depth], to_x)
            hop.start()
            hop.wait()
            half = sa_ref.at[c]
            hop = remote(half, half, ssend.at[depth + 1], srecv.at[depth + 1], to_c)
            hop.start()
            hop.wait()
            end_gather(depth, ta_ref, z, c, token_sems, token_state)
    relay(depth - 1)
    for d in range(depth):
        if d % 2 == 0:
            x_copies[d].wait_recv()
        else:
            y_copies[d].wait_recv()
        d_copies[d].wait_recv()
        y_copies[d].wait_send()
        x_copies[d].wait_send()
        d_copies[d].wait_send()
    for copy in z_copies:
        copy.wait_send()
    keep.wait()


def spread_weights(depth, blocks, scale_block, own_rows):
    rows, width = blocks.shape[1:]
    dma = pltpu.SemaphoreType.DMA
    return pl.pallas_call(
        functools.partial(weights_kernel, depth),
        out_shape=(
            jax.ShapeDtypeStruct((2, rows, depth * 2 * width), jnp.bfloat16),
            jax.ShapeDtypeStruct((CORES, 2, 2, depth) + scale_block.shape, jnp.float32),
            jax.ShapeDtypeStruct((depth, CORES) + own_rows.shape, jnp.bfloat16),
        ),
        in_specs=[ANY, ANY, ANY],
        out_specs=(ANY, ANY, ANY),
        scratch_shapes=[dma((depth,)) for _ in range(8)]
        + [dma((depth + 2,)), dma((depth + 2,))]
        + [dma((depth,)) for _ in range(4)]
        + [dma((3,))],
        compiler_params=pltpu.CompilerParams(collective_id=0, has_side_effects=True),
        name="spread_weights",
    )(blocks, scale_block, own_rows)


def join_kernel(depth, gather, part_ref, res_ref, scale_ref, gain_ref, shift_ref, out_ref, *rest):
    if gather:
        ta_ref, rest = rest[0], rest[1:]
    half, sums, got, hsend, hrecv, rsend, rrecv = rest[:7]
    z, c = lax.axis_index("z"), lax.axis_index("c")
    greet(depth, ("c",))
    order = list(range(1, depth)) + [0]
    halves = {}
    for d in order:
        target = lax.rem(z + d, depth)
        halves[d] = remote(part_ref.at[target, 1 - c], half.at[d], hsend.at[d], hrecv.at[d], {"c": 1 - c})
        halves[d].start()
    shares = []
    for d in order[:-1]:
        target = lax.rem(z + d, depth)
        halves[d].wait_recv()
        both = part_ref[target, c].astype(jnp.float32) + half[d].astype(jnp.float32)
        sums[d] = both.astype(jnp.bfloat16)
        copy = remote(sums.at[d], got.at[d], rsend.at[d], rrecv.at[d], {"z": target})
        copy.start()
        shares.append(copy)
    halves[0].wait_recv()
    total = part_ref[z, c].astype(jnp.float32) + half[0].astype(jnp.float32)
    for d in range(1, depth):
        shares[d - 1].wait_recv()
        total = total + got[d].astype(jnp.float32)
    summed = RESIDUAL_SCALE * res_ref[...].astype(jnp.float32) + total * scale_ref[...]
    count = summed.shape[1]
    average = jnp.sum(summed, -1, keepdims=True) / count
    mean_square = jnp.sum(summed * summed, -1, keepdims=True) / count
    variance = mean_square - average * average
    normed = (summed - average) * lax.rsqrt(variance + EPSILON) * gain_ref[...] + shift_ref[...]
    out_ref[...] = normed.astype(jnp.bfloat16)
    if gather:
        sems = rest[7:]
        state = start_gather(depth, out_ref, ta_ref, z, c, sems)
        end_gather(depth, ta_ref, z, c, sems, state)
    for d in range(depth):
        halves[d].wait_send()
    for copy in shares:
        copy.wait_send()


def join(depth, gather, number, part, residual, scale, gain, shift):
    rows, features = residual.shape
    dma = pltpu.SemaphoreType.DMA
    block = pltpu.VMEM((depth, rows, features), jnp.bfloat16)
    out_shape = [jax.ShapeDtypeStruct((rows, features), jnp.bfloat16)]
    out_specs = [VMEM]
    scratch = [block, block, block] + [dma((depth,)) for _ in range(4)]
    if gather:
        out_shape.append(jax.ShapeDtypeStruct((depth, CORES, rows, features), jnp.bfloat16))
        out_specs.append(ANY)
        scratch += [dma((depth,)) for _ in range(4)] + [dma]
    return pl.pallas_call(
        functools.partial(join_kernel, depth, gather),
        out_shape=tuple(out_shape),
        in_specs=[VMEM] * 5,
        out_specs=tuple(out_specs),
        scratch_shapes=scratch,
        compiler_params=pltpu.CompilerParams(collective_id=number, has_side_effects=True),
        name=f"join_{number}",
    )(part, residual, scale[None], gain[None], shift[None])


def dot_last(left, right):
    return lax.dot_general(left, right, (((1,), (1,)), ((), ())), preferred_element_type=jnp.float32)


def dot_first(left, right):
    return lax.dot_general(left, right, (((0,), (0,)), ((), ())), preferred_element_type=jnp.float32)


def column_plan(
    depth, tokens, gate_weight, up_weight, down_weight, gate_scale, up_scale, down_scale,
    bgate_weight, cgate_weight, value_weight, bgate_scale, cgate_scale, value_scale, conv_taps,
    mixout_weight, mixout_scale, first_gain, first_shift, mixer_gain, mixer_shift, last_gain, last_shift,
):
    z, c = lax.axis_index("z"), lax.axis_index("c")
    own = lax.all_to_all(tokens, ("x", "c"), 0, 1, tiled=True)
    rows, features = own.shape

    def cut(matrix):
        return matrix.astype(jnp.bfloat16).reshape(depth, -1, matrix.shape[1])

    blocks = jnp.concatenate(
        [cut(gate_weight.T), cut(up_weight.T), cut(down_weight)]
        + [cut(m.T) for m in (bgate_weight, cgate_weight, value_weight)]
        + [cut(mixout_weight)],
        axis=1,
    )
    units = gate_weight.shape[1] // depth
    channels = bgate_weight.shape[1] // depth
    pieces = (gate_scale, up_scale, down_scale, bgate_scale, cgate_scale, value_scale, mixout_scale)
    flat = jnp.concatenate([piece.reshape(-1) for piece in pieces])
    flat = jnp.pad(flat, (0, -flat.shape[0] % 1024)).reshape(-1, 128)
    kept, scales, gathered = spread_weights(depth, blocks, flat, own)
    scales = scales.reshape(scales.shape[:4] + (-1,))
    mine = lax.dynamic_index_in_dim(lax.dynamic_index_in_dim(scales, c, 0, False), z, 2, False)
    edges = [0]
    for piece in pieces:
        edges.append(edges[-1] + piece.shape[1])

    def unit_scale(k):
        return mine[:, :, edges[k] : edges[k + 1]].reshape(2, -1)

    def feature_scale(k):
        return scales[..., edges[k] : edges[k + 1]].transpose(1, 0, 3, 2, 4).reshape(-1)

    gate_cols, up_cols = unit_scale(0), unit_scale(1)
    bgate_cols, cgate_cols, value_cols = unit_scale(3), unit_scale(4), unit_scale(5)
    down_cols, mixout_cols = HALF_STEP * feature_scale(2), feature_scale(6)
    taps = conv_taps.reshape(TAPS, 2, CORES, depth, channels)
    taps = lax.dynamic_index_in_dim(lax.dynamic_index_in_dim(taps, c, 2, False), z, 2, False)

    def shares(total):
        return total.astype(jnp.bfloat16).reshape(depth, CORES, rows, features)

    def channel_mix(whole):
        inputs = whole.reshape(-1, features)
        total = 0.0
        for k in range(2):
            sums = dot_last(kept[k, : 2 * units], inputs)
            gate_sum = sums[:units] * gate_cols[k][:, None]
            up_sum = sums[units:] * up_cols[k][:, None]
            hidden = (jax.nn.silu(gate_sum) * up_sum).astype(jnp.bfloat16)
            total = total + dot_first(hidden, kept[k, 2 * units : 3 * units])
        return shares(total)

    def token_mix(whole):
        inputs = whole.reshape(-1, features)
        base = 3 * units
        total = 0.0
        for k in range(2):
            sums = dot_last(inputs, kept[k, base : base + 3 * channels])
            outgate = sums[:, :channels] * bgate_cols[k]
            ingate = sums[:, channels : 2 * channels] * cgate_cols[k]
            values = sums[:, 2 * channels :] * value_cols[k]
            mixed = (ingate * values).reshape(-1, LENGTH, channels)
            padded = jnp.pad(mixed, ((0, 0), (TAPS - 1, 0), (0, 0)))
            convolved = jnp.zeros(mixed.shape, jnp.float32)
            for tap in range(TAPS):
                convolved = convolved + taps[tap, k] * padded[:, tap : tap + LENGTH]
            gated = (outgate * convolved.reshape(-1, channels)).astype(jnp.bfloat16)
            total = total + jnp.dot(
                gated, kept[k, base + 3 * channels :], preferred_element_type=jnp.float32
            )
        return shares(total)

    first, gathered = join(depth, True, 1, channel_mix(gathered), own, down_cols, first_gain, first_shift)
    second, gathered = join(depth, True, 2, token_mix(gathered), first, mixout_cols, mixer_gain, mixer_shift)
    (last,) = join(depth, False, 3, channel_mix(gathered), second, down_cols, last_gain, last_shift)
    return lax.all_to_all(last, ("x", "c"), 1, 0, tiled=True)


def add_rows(gathered, shard_piece):
    return jnp.dot(gathered, shard_piece, preferred_element_type=jnp.float32)


def features(inputs):
    return lax.all_gather(inputs, "tp", axis=1, tiled=True)


def post_norm(residual, branch, norm_gain, norm_shift):
    summed = RESIDUAL_SCALE * residual.astype(jnp.float32) + branch
    moments = lax.psum((jnp.sum(summed, -1), jnp.sum(summed * summed, -1)), "tp")
    feature_total = summed.shape[1] * lax.axis_size("tp")
    average = (moments[0] / feature_total)[:, None]
    mean_square = (moments[1] / feature_total)[:, None]
    variance = mean_square - average * average
    return ((summed - average) * lax.rsqrt(variance + EPSILON) * norm_gain + norm_shift).astype(
        jnp.bfloat16
    )


def spread_back(weight_cols, left_rows):
    return (
        lax.psum_scatter(
            lax.dot_general(
                weight_cols, left_rows, (((0,), (1,)), ((), ())), preferred_element_type=jnp.float32
            ).astype(jnp.bfloat16),
            "tp",
            scatter_dimension=0,
            tiled=True,
        )
        .astype(jnp.float32)
        .T
    )


def shards(
    tokens,
    gate_weight,
    up_weight,
    down_weight,
    gate_scale,
    up_scale,
    down_scale,
    bgate_weight,
    cgate_weight,
    value_weight,
    bgate_scale,
    cgate_scale,
    value_scale,
    conv_taps,
    mixout_weight,
    mixout_scale,
    first_gain,
    first_shift,
    mixer_gain,
    mixer_shift,
    last_gain,
    last_shift,
):
    scales = (
        lax.all_gather(gate_scale, "fs", axis=1, tiled=True),
        lax.all_gather(up_scale, "fs", axis=1, tiled=True),
        lax.all_gather(down_scale, "fs", axis=1, tiled=True),
        lax.all_gather(bgate_scale, "fs", axis=1, tiled=True),
        lax.all_gather(cgate_scale, "fs", axis=1, tiled=True),
        lax.all_gather(value_scale, "fs", axis=1, tiled=True),
        lax.all_gather(mixout_scale, "fs", axis=1, tiled=True),
    )
    gate_cols, up_cols, down_cols, bgate_cols, cgate_cols, value_cols, mixout_cols = [
        scale_row.reshape(-1) for scale_row in scales
    ]
    tp_index = lax.axis_index("tp")
    columns = tokens.shape[1]

    def own_part(vector):
        return lax.dynamic_slice_in_dim(vector, tp_index * columns, columns)

    gate_low = gate_weight.astype(jnp.bfloat16)
    up_low = up_weight.astype(jnp.bfloat16)
    down_low = down_weight.astype(jnp.bfloat16)
    kept_gate, kept_up = (
        lax.all_gather(gate_low, "fs", axis=0, tiled=True),
        lax.all_gather(up_low, "fs", axis=0, tiled=True),
    )
    kept_down = lax.all_gather(down_low, "fs", axis=1, tiled=True)

    def channel_mix(gathered):
        gate_sum = jnp.dot(gathered, kept_gate, preferred_element_type=jnp.float32)
        up_sum = jnp.dot(gathered, kept_up, preferred_element_type=jnp.float32)
        hidden = (jax.nn.silu(gate_sum * gate_cols) * (up_sum * up_cols)).astype(jnp.bfloat16)
        return HALF_STEP * (spread_back(kept_down, hidden) * down_cols)

    first = post_norm(
        tokens, channel_mix(features(tokens)), own_part(first_gain), own_part(first_shift)
    )
    gathered = features(first)
    bgate_low = bgate_weight.astype(jnp.bfloat16)
    channels = bgate_low.shape[1]
    outgate = add_rows(gathered, lax.all_gather(bgate_low, "fs", axis=0, tiled=True))
    ingate = add_rows(
        gathered, lax.all_gather(cgate_weight.astype(jnp.bfloat16), "fs", axis=0, tiled=True)
    )
    values = add_rows(
        gathered, lax.all_gather(value_weight.astype(jnp.bfloat16), "fs", axis=0, tiled=True)
    )
    tap_weights = lax.dynamic_slice_in_dim(conv_taps, tp_index * channels, channels, 1)
    mixed = (ingate * cgate_cols * (values * value_cols)).reshape(-1, LENGTH, channels)
    padded = jnp.pad(mixed, ((0, 0), (TAPS - 1, 0), (0, 0)))
    convolved = jnp.zeros(mixed.shape, jnp.float32)
    for tap_index in range(TAPS):
        convolved = convolved + tap_weights[tap_index] * padded[:, tap_index : tap_index + LENGTH]
    gated = (outgate * bgate_cols * convolved.reshape(-1, channels)).astype(jnp.bfloat16)
    mix_full = lax.all_gather(mixout_weight.astype(jnp.bfloat16), "fs", axis=1, tiled=True)
    second = post_norm(
        first,
        spread_back(mix_full, gated) * mixout_cols,
        own_part(mixer_gain),
        own_part(mixer_shift),
    )
    return post_norm(
        second, channel_mix(features(second)), own_part(last_gain), own_part(last_shift)
    )


def solution(mesh):
    in_specs = (
        P("fs", "tp"),
        P("fs", "tp"),
        P("fs", "tp"),
        P("tp", "fs"),
        P("tp", "fs"),
        P("tp", "fs"),
        P("tp", "fs"),
        P("fs", "tp"),
        P("fs", "tp"),
        P("fs", "tp"),
        P("tp", "fs"),
        P("tp", "fs"),
        P("tp", "fs"),
        P(),
        P("tp", "fs"),
        P("tp", "fs"),
        P(),
        P(),
        P(),
        P(),
        P(),
        P(),
    )
    out_specs = P("fs", "tp")
    across = mesh.shape["tp"] // CORES
    if across == 2 and mesh.shape["fs"] % 2 == 0 and mesh.shape["fs"] > 2:
        depth = mesh.shape["fs"] // 2
        fine = Mesh(mesh.devices.reshape(depth, 2, 2, CORES), ("z", "y", "x", "c"))
        names = {"fs": ("z", "y"), "tp": ("x", "c")}

        def split(spec):
            return P(*(names.get(name) for name in spec))

        return jax.shard_map(
            functools.partial(column_plan, depth),
            mesh=fine,
            in_specs=tuple(split(spec) for spec in in_specs),
            out_specs=split(out_specs),
            check_vma=False,
        )
    return jax.shard_map(shards, mesh=mesh, in_specs=in_specs, out_specs=out_specs, check_vma=False)
```

```python
import functools

import jax
import jax.numpy as jnp
from jax import lax
from jax.experimental import pallas as pl
from jax.experimental.pallas import tpu as pltpu
from jax.sharding import Mesh
from jax.sharding import PartitionSpec as P

TAPS = 3
LENGTH = 128
CORES = 2

RESIDUAL_SCALE = 1.4142135623730951
HALF_STEP = 0.5
EPSILON = 1e-05
BY_AXIS = pl.DeviceIdType.MESH
ANY = pl.BlockSpec(memory_space=pl.ANY)
VMEM = pl.BlockSpec(memory_space=pltpu.VMEM)


def greet(depth, axes):
    barrier = pltpu.get_barrier_semaphore()
    z = lax.axis_index("z")
    targets = [{"z": lax.rem(z + d, depth)} for d in range(1, depth)]
    targets += [{axis: 1 - lax.axis_index(axis)} for axis in axes]
    for target in targets:
        pl.semaphore_signal(barrier, inc=1, device_id=target, device_id_type=BY_AXIS)
    pl.semaphore_wait(barrier, len(targets))


def remote(src, dst, send, recv, target):
    return pltpu.make_async_remote_copy(
        src_ref=src, dst_ref=dst, send_sem=send, recv_sem=recv, device_id=target, device_id_type=BY_AXIS
    )


def block_place(ref, px, pz, py, width):
    start = pl.multiple_of((pz * 2 + py) * width, width)
    return ref.at[:, px, :, pl.ds(start, width)]


def weights_kernel(
    depth, w_ref, m_ref, s_ref, t_ref, g_ref, held_ref, sa_ref, ta_ref,
    zsend, zrecv, ysend, yrecv, xsend, xrecv, dsend, drecv, msend, mrecv,
    ssend, srecv, tzsend, tzrecv, tcsend, tcrecv, local,
):
    z, y, x, c = (lax.axis_index(axis) for axis in ("z", "y", "x", "c"))
    width = w_ref.shape[-1]
    greet(depth, ("y", "x", "c"))

    def place(px, pz, py):
        return block_place(g_ref, px, pz, py, width)

    to_x, to_y, to_c = {"x": 1 - x}, {"y": 1 - y}, {"c": 1 - c}
    scale_sends, token_sends, z_copies, m_copies = [], [], [], []
    keeps = [
        pltpu.make_async_copy(s_ref, sa_ref.at[c, x, y, z], local.at[0]),
        pltpu.make_async_copy(t_ref, ta_ref.at[0, c], local.at[1]),
        pltpu.make_async_copy(w_ref.at[z], place(x, z, y), local.at[2]),
        pltpu.make_async_copy(m_ref.at[z], held_ref.at[0], local.at[3]),
    ]
    for copy in keeps:
        copy.start()
    beside = [remote(t_ref, ta_ref.at[0, c], tcsend.at[0], tcrecv.at[0], to_c)]
    beside[0].start()
    own_y = remote(w_ref.at[z], place(x, z, y), ysend.at[0], yrecv.at[0], to_y)
    own_x = remote(w_ref.at[z], place(x, z, y), xsend.at[0], xrecv.at[0], to_x)
    own_y.start()
    own_x.start()
    y_copies, x_copies, d_copies = [own_y], [own_x], []
    for d in range(1, depth):
        target = {"z": lax.rem(z + d, depth)}
        scale_sends.append(remote(s_ref, sa_ref.at[c, x, y, z], ssend.at[d], srecv.at[d], target))
        scale_sends[-1].start()
    for d in range(1, depth):
        target = lax.rem(z + d, depth)
        z_copies.append(remote(w_ref.at[target], place(x, z, y), zsend.at[d], zrecv.at[d], {"z": target}))
        z_copies[-1].start()
    for d in range(1, depth):
        target = {"z": lax.rem(z + d, depth)}
        token_sends.append(remote(t_ref, ta_ref.at[d, c], tzsend.at[d], tzrecv.at[d], target))
        token_sends[-1].start()
    for d in range(1, depth):
        target = lax.rem(z + d, depth)
        m_copies.append(remote(m_ref.at[target], held_ref.at[d], msend.at[d], mrecv.at[d], {"z": target}))
        m_copies[-1].start()

    def relay(d):
        source = lax.rem(z - d + depth, depth)
        if d % 2 == 0:
            y_copies[d].wait_recv()
            block = place(x, source, 1 - y)
            copy = remote(block, block, dsend.at[d], drecv.at[d], to_x)
        else:
            x_copies[d].wait_recv()
            block = place(1 - x, source, y)
            copy = remote(block, block, dsend.at[d], drecv.at[d], to_y)
        copy.start()
        d_copies.append(copy)

    keeps[0].wait()
    for copy in scale_sends:
        copy.wait()
    hops = (sa_ref.at[c, x, y], sa_ref.at[c, x], sa_ref.at[c])
    for k, (part, target) in enumerate(zip(hops, (to_y, to_x, to_c))):
        slot = (0, depth, depth + 1)[k]
        hop = remote(part, part, ssend.at[slot], srecv.at[slot], target)
        hop.start()
        hop.wait()
    for d in range(1, depth):
        block = place(x, lax.rem(z - d + depth, depth), y)
        z_copies[d - 1].wait_recv()
        ycopy = remote(block, block, ysend.at[d], yrecv.at[d], to_y)
        xcopy = remote(block, block, xsend.at[d], xrecv.at[d], to_x)
        ycopy.start()
        xcopy.start()
        y_copies.append(ycopy)
        x_copies.append(xcopy)
        relay(d - 1)
    relay(depth - 1)
    for d in range(1, depth):
        token_sends[d - 1].wait_recv()
        copy = remote(ta_ref.at[d, c], ta_ref.at[d, c], tcsend.at[d], tcrecv.at[d], to_c)
        copy.start()
        beside.append(copy)
    for d in range(depth):
        if d % 2 == 0:
            x_copies[d].wait_recv()
        else:
            y_copies[d].wait_recv()
        d_copies[d].wait_recv()
        y_copies[d].wait_send()
        x_copies[d].wait_send()
        d_copies[d].wait_send()
        beside[d].wait()
    for copy in m_copies:
        copy.wait()
    for copy in z_copies + token_sends:
        copy.wait_send()
    for copy in keeps[1:]:
        copy.wait()


def spread_weights(depth, blocks, mixer_blocks, scale_block, own_rows):
    mats, rows, width = blocks.shape[1:]
    dma = pltpu.SemaphoreType.DMA
    return pl.pallas_call(
        functools.partial(weights_kernel, depth),
        out_shape=(
            jax.ShapeDtypeStruct((mats, 2, rows, depth * 2 * width), jnp.bfloat16),
            jax.ShapeDtypeStruct(mixer_blocks.shape, jnp.bfloat16),
            jax.ShapeDtypeStruct((CORES, 2, 2, depth) + scale_block.shape, jnp.float32),
            jax.ShapeDtypeStruct((depth, CORES) + own_rows.shape, jnp.bfloat16),
        ),
        in_specs=[ANY] * 4,
        out_specs=(ANY,) * 4,
        scratch_shapes=[dma((depth,)) for _ in range(10)]
        + [dma((depth + 2,)), dma((depth + 2,))]
        + [dma((depth,)) for _ in range(4)]
        + [dma((4,))],
        compiler_params=pltpu.CompilerParams(collective_id=0, has_side_effects=True),
        name="spread_weights",
    )(blocks, mixer_blocks, scale_block, own_rows)


def dot_last(left, right):
    return lax.dot_general(left, right, (((1,), (1,)), ((), ())), preferred_element_type=jnp.float32)


def merged(ref, k):
    two, rows, features = ref.shape[1:]
    return ref[k].reshape(two * rows, features)


def feed_chunk(inputs, weights, factors, taps):
    gate_sum = dot_last(inputs, merged(weights, 0)) * factors[0:1]
    up_sum = dot_last(inputs, merged(weights, 1)) * factors[1:2]
    hidden = (gate_sum / (1.0 + jnp.exp(-gate_sum)) * up_sum).astype(jnp.bfloat16)
    return jnp.dot(hidden, merged(weights, 2), preferred_element_type=jnp.float32)


def mixer_chunk(inputs, weights, factors, taps):
    outgate = dot_last(inputs, merged(weights, 0)) * factors[0:1]
    ingate = dot_last(inputs, merged(weights, 1)) * factors[1:2]
    values = dot_last(inputs, merged(weights, 2)) * factors[2:3]
    mixed = ingate * values
    position = lax.rem(lax.broadcasted_iota(jnp.int32, mixed.shape, 0), LENGTH)
    convolved = taps[TAPS - 1 : TAPS] * mixed
    for back in range(1, TAPS):
        earlier = jnp.where(position >= back, pltpu.roll(mixed, back, 0), 0.0)
        convolved = convolved + taps[TAPS - 1 - back : TAPS - back] * earlier
    gated = (outgate * convolved).astype(jnp.bfloat16)
    return jnp.dot(gated, merged(weights, 3), preferred_element_type=jnp.float32)


def stage_kernel(depth, chunk, first, *refs):
    refs = list(refs)
    take = lambda n: [refs.pop(0) for _ in range(n)]
    w_ref, f_ref, k_ref, own_ref, scale_ref, gain_ref, shift_ref = take(7)
    if first:
        whole, held_ref = take(2)
        out_ref, m_ref = take(2)
    else:
        (out_ref,) = take(1)
    part, half, sums, got, hsend, hrecv, rsend, rrecv = take(8)
    z, c = lax.axis_index("z"), lax.axis_index("c")
    to_c = {"c": 1 - c}
    if first:
        ysend, yrecv, xsend, xrecv, dsend, drecv, local = take(7)
        y, x = lax.axis_index("y"), lax.axis_index("x")
        greet(depth, ("y", "x", "c"))
        width = held_ref.shape[-1]
        y_copies, x_copies, d_copies, keeps = [], [], [], []
        for d in range(depth):
            block = block_place(m_ref, x, lax.rem(z - d + depth, depth), y, width)
            y_copies.append(remote(held_ref.at[d], block, ysend.at[d], yrecv.at[d], {"y": 1 - y}))
            x_copies.append(remote(held_ref.at[d], block, xsend.at[d], xrecv.at[d], {"x": 1 - x}))
            keeps.append(pltpu.make_async_copy(held_ref.at[d], block, local.at[d]))
            y_copies[d].start()
            x_copies[d].start()
            keeps[d].start()
    else:
        whole, zsend, zrecv, csend, crecv = take(5)
        greet(depth, ("c",))
        beside = remote(own_ref, whole.at[0, c], csend.at[0], crecv.at[0], to_c)
        beside.start()
        across = []
        for d in range(1, depth):
            target = {"z": lax.rem(z + d, depth)}
            across.append(remote(own_ref, whole.at[d, c], zsend.at[d], zrecv.at[d], target))
            across[-1].start()
        whole[0, c] = own_ref[...]

    def share(d):
        target = {"z": lax.rem(z - d + depth, depth)}
        return remote(sums.at[d], got.at[d], rsend.at[d], rrecv.at[d], target)

    def handover(d):
        return remote(part.at[d, 1 - c], half.at[d], hsend.at[d], hrecv.at[d], to_c)

    def forward(d):
        return remote(whole.at[d, c], whole.at[d, c], csend.at[d], crecv.at[d], to_c)

    def step(i, carry):
        d = lax.rem(i + 1, depth) if first else i
        if not first:

            @pl.when(d > 0)
            def _():
                remote(own_ref, whole.at[d, c], zsend.at[d], zrecv.at[d], {"z": z}).wait_recv()
                forward(d).start()

            forward(d).wait_recv()
        rows = own_ref.shape[0]
        inputs = whole[d].reshape(CORES * rows, -1)
        total = chunk(inputs, w_ref, f_ref[...], k_ref[...])
        part[d] = total.astype(jnp.bfloat16).reshape(part.shape[1:])
        handover(d).start()
        handover(d).wait_recv()

        @pl.when(d > 0)
        def _():
            both = part[d, c].astype(jnp.float32) + half[d].astype(jnp.float32)
            sums[d] = both.astype(jnp.bfloat16)
            share(d).start()

        return carry

    lax.fori_loop(0, depth, step, 0)
    if first:
        for d in range(depth):
            source = lax.rem(z - d + depth, depth)
            if d % 2 == 0:
                y_copies[d].wait_recv()
                block = block_place(m_ref, x, source, 1 - y, width)
                copy = remote(block, block, dsend.at[d], drecv.at[d], {"x": 1 - x})
            else:
                x_copies[d].wait_recv()
                block = block_place(m_ref, 1 - x, source, y, width)
                copy = remote(block, block, dsend.at[d], drecv.at[d], {"y": 1 - y})
            copy.start()
            d_copies.append(copy)
    total = part[0, c].astype(jnp.float32) + half[0].astype(jnp.float32)
    for d in range(1, depth):
        share(d).wait_recv()
        total = total + got[d].astype(jnp.float32)
    summed = RESIDUAL_SCALE * own_ref[...].astype(jnp.float32) + total * scale_ref[...]
    count = summed.shape[1]
    average = jnp.sum(summed, -1, keepdims=True) / count
    mean_square = jnp.sum(summed * summed, -1, keepdims=True) / count
    variance = mean_square - average * average
    normed = (summed - average) * lax.rsqrt(variance + EPSILON) * gain_ref[...] + shift_ref[...]
    out_ref[...] = normed.astype(jnp.bfloat16)
    for d in range(depth):
        handover(d).wait_send()
        if d > 0:
            share(d).wait_send()
    if first:
        for d in range(depth):
            (x_copies if d % 2 == 0 else y_copies)[d].wait_recv()
            for copy in (y_copies[d], x_copies[d]):
                copy.wait_send()
            d_copies[d].wait()
            keeps[d].wait()
    else:
        beside.wait_send()
        for d in range(1, depth):
            forward(d).wait_send()
            across[d - 1].wait_send()


def stage(depth, number, chunk, weights, factors, taps, own, scale, gain, shift, whole=None, held=None):
    rows, features = own.shape
    first = whole is not None
    dma = pltpu.SemaphoreType.DMA
    block = pltpu.VMEM((depth, rows, features), jnp.bfloat16)
    pair = pltpu.VMEM((depth, CORES, rows, features), jnp.bfloat16)
    operands = [weights, factors, taps, own, scale[None], gain[None], shift[None]]
    in_specs = [VMEM] * 7
    out_shape = [jax.ShapeDtypeStruct((rows, features), jnp.bfloat16)]
    out_specs = [VMEM]
    scratch = [pair, block, block, block] + [dma((depth,)) for _ in range(4)]
    if first:
        operands += [whole, held]
        in_specs += [VMEM, ANY]
        mats, part_rows, width = held.shape[1:]
        out_shape.append(jax.ShapeDtypeStruct((mats, 2, part_rows, depth * 2 * width), jnp.bfloat16))
        out_specs.append(ANY)
        scratch += [dma((depth,)) for _ in range(7)]
    else:
        scratch += [pair] + [dma((depth,)) for _ in range(4)]
    return pl.pallas_call(
        functools.partial(stage_kernel, depth, chunk, first),
        out_shape=tuple(out_shape),
        in_specs=in_specs,
        out_specs=tuple(out_specs),
        scratch_shapes=scratch,
        compiler_params=pltpu.CompilerParams(
            collective_id=number, has_side_effects=True, vmem_limit_bytes=40 * 1024 * 1024
        ),
        name=f"stage_{number}",
    )(*operands)


def column_plan(
    depth, tokens, gate_weight, up_weight, down_weight, gate_scale, up_scale, down_scale,
    bgate_weight, cgate_weight, value_weight, bgate_scale, cgate_scale, value_scale, conv_taps,
    mixout_weight, mixout_scale, first_gain, first_shift, mixer_gain, mixer_shift, last_gain, last_shift,
):
    z, c = lax.axis_index("z"), lax.axis_index("c")
    own = lax.all_to_all(tokens, ("x", "c"), 0, 1, tiled=True)

    def cut(matrix):
        return matrix.astype(jnp.bfloat16).reshape(depth, -1, matrix.shape[1])

    blocks = jnp.stack([cut(gate_weight.T), cut(up_weight.T), cut(down_weight)], axis=1)
    mixer_blocks = jnp.stack(
        [cut(m.T) for m in (bgate_weight, cgate_weight, value_weight)] + [cut(mixout_weight)], axis=1
    )
    channels = bgate_weight.shape[1] // depth
    pieces = (gate_scale, up_scale, down_scale, bgate_scale, cgate_scale, value_scale, mixout_scale)
    flat = jnp.concatenate([piece.reshape(-1) for piece in pieces])
    flat = jnp.pad(flat, (0, -flat.shape[0] % 1024)).reshape(-1, 128)
    feed_weights, held, scales, whole = spread_weights(depth, blocks, mixer_blocks, flat, own)
    scales = scales.reshape(scales.shape[:4] + (-1,))
    mine = lax.dynamic_index_in_dim(lax.dynamic_index_in_dim(scales, c, 0, False), z, 2, False)
    edges = [0]
    for piece in pieces:
        edges.append(edges[-1] + piece.shape[1])

    def unit_scale(k):
        return mine[:, :, edges[k] : edges[k + 1]].reshape(-1)

    def feature_scale(k):
        return scales[..., edges[k] : edges[k + 1]].transpose(1, 0, 3, 2, 4).reshape(-1)

    feed_factors = jnp.stack([unit_scale(0), unit_scale(1)])
    mixer_factors = jnp.stack([unit_scale(3), unit_scale(4), unit_scale(5)])
    down_cols, mixout_cols = HALF_STEP * feature_scale(2), feature_scale(6)
    taps = conv_taps.reshape(TAPS, 2, CORES, depth, channels)
    taps = lax.dynamic_index_in_dim(lax.dynamic_index_in_dim(taps, c, 2, False), z, 2, False)
    taps = taps.reshape(TAPS, -1)

    first, mixer_weights = stage(
        depth, 1, feed_chunk, feed_weights, feed_factors, taps, own, down_cols, first_gain, first_shift, whole, held
    )
    (second,) = stage(
        depth, 2, mixer_chunk, mixer_weights, mixer_factors, taps, first, mixout_cols, mixer_gain, mixer_shift
    )
    (last,) = stage(
        depth, 3, feed_chunk, feed_weights, feed_factors, taps, second, down_cols, last_gain, last_shift
    )
    return lax.all_to_all(last, ("x", "c"), 1, 0, tiled=True)


def add_rows(gathered, shard_piece):
    return jnp.dot(gathered, shard_piece, preferred_element_type=jnp.float32)


def features(inputs):
    return lax.all_gather(inputs, "tp", axis=1, tiled=True)


def post_norm(residual, branch, norm_gain, norm_shift):
    summed = RESIDUAL_SCALE * residual.astype(jnp.float32) + branch
    moments = lax.psum((jnp.sum(summed, -1), jnp.sum(summed * summed, -1)), "tp")
    feature_total = summed.shape[1] * lax.axis_size("tp")
    average = (moments[0] / feature_total)[:, None]
    mean_square = (moments[1] / feature_total)[:, None]
    variance = mean_square - average * average
    return ((summed - average) * lax.rsqrt(variance + EPSILON) * norm_gain + norm_shift).astype(
        jnp.bfloat16
    )


def spread_back(weight_cols, left_rows):
    return (
        lax.psum_scatter(
            lax.dot_general(
                weight_cols, left_rows, (((0,), (1,)), ((), ())), preferred_element_type=jnp.float32
            ).astype(jnp.bfloat16),
            "tp",
            scatter_dimension=0,
            tiled=True,
        )
        .astype(jnp.float32)
        .T
    )


def shards(
    tokens,
    gate_weight,
    up_weight,
    down_weight,
    gate_scale,
    up_scale,
    down_scale,
    bgate_weight,
    cgate_weight,
    value_weight,
    bgate_scale,
    cgate_scale,
    value_scale,
    conv_taps,
    mixout_weight,
    mixout_scale,
    first_gain,
    first_shift,
    mixer_gain,
    mixer_shift,
    last_gain,
    last_shift,
):
    scales = (
        lax.all_gather(gate_scale, "fs", axis=1, tiled=True),
        lax.all_gather(up_scale, "fs", axis=1, tiled=True),
        lax.all_gather(down_scale, "fs", axis=1, tiled=True),
        lax.all_gather(bgate_scale, "fs", axis=1, tiled=True),
        lax.all_gather(cgate_scale, "fs", axis=1, tiled=True),
        lax.all_gather(value_scale, "fs", axis=1, tiled=True),
        lax.all_gather(mixout_scale, "fs", axis=1, tiled=True),
    )
    gate_cols, up_cols, down_cols, bgate_cols, cgate_cols, value_cols, mixout_cols = [
        scale_row.reshape(-1) for scale_row in scales
    ]
    tp_index = lax.axis_index("tp")
    columns = tokens.shape[1]

    def own_part(vector):
        return lax.dynamic_slice_in_dim(vector, tp_index * columns, columns)

    gate_low = gate_weight.astype(jnp.bfloat16)
    up_low = up_weight.astype(jnp.bfloat16)
    down_low = down_weight.astype(jnp.bfloat16)
    kept_gate, kept_up = (
        lax.all_gather(gate_low, "fs", axis=0, tiled=True),
        lax.all_gather(up_low, "fs", axis=0, tiled=True),
    )
    kept_down = lax.all_gather(down_low, "fs", axis=1, tiled=True)

    def channel_mix(gathered):
        gate_sum = jnp.dot(gathered, kept_gate, preferred_element_type=jnp.float32)
        up_sum = jnp.dot(gathered, kept_up, preferred_element_type=jnp.float32)
        hidden = (jax.nn.silu(gate_sum * gate_cols) * (up_sum * up_cols)).astype(jnp.bfloat16)
        return HALF_STEP * (spread_back(kept_down, hidden) * down_cols)

    first = post_norm(
        tokens, channel_mix(features(tokens)), own_part(first_gain), own_part(first_shift)
    )
    gathered = features(first)
    bgate_low = bgate_weight.astype(jnp.bfloat16)
    channels = bgate_low.shape[1]
    outgate = add_rows(gathered, lax.all_gather(bgate_low, "fs", axis=0, tiled=True))
    ingate = add_rows(
        gathered, lax.all_gather(cgate_weight.astype(jnp.bfloat16), "fs", axis=0, tiled=True)
    )
    values = add_rows(
        gathered, lax.all_gather(value_weight.astype(jnp.bfloat16), "fs", axis=0, tiled=True)
    )
    tap_weights = lax.dynamic_slice_in_dim(conv_taps, tp_index * channels, channels, 1)
    mixed = (ingate * cgate_cols * (values * value_cols)).reshape(-1, LENGTH, channels)
    padded = jnp.pad(mixed, ((0, 0), (TAPS - 1, 0), (0, 0)))
    convolved = jnp.zeros(mixed.shape, jnp.float32)
    for tap_index in range(TAPS):
        convolved = convolved + tap_weights[tap_index] * padded[:, tap_index : tap_index + LENGTH]
    gated = (outgate * bgate_cols * convolved.reshape(-1, channels)).astype(jnp.bfloat16)
    mix_full = lax.all_gather(mixout_weight.astype(jnp.bfloat16), "fs", axis=1, tiled=True)
    second = post_norm(
        first,
        spread_back(mix_full, gated) * mixout_cols,
        own_part(mixer_gain),
        own_part(mixer_shift),
    )
    return post_norm(
        second, channel_mix(features(second)), own_part(last_gain), own_part(last_shift)
    )


def solution(mesh):
    in_specs = (
        P("fs", "tp"),
        P("fs", "tp"),
        P("fs", "tp"),
        P("tp", "fs"),
        P("tp", "fs"),
        P("tp", "fs"),
        P("tp", "fs"),
        P("fs", "tp"),
        P("fs", "tp"),
        P("fs", "tp"),
        P("tp", "fs"),
        P("tp", "fs"),
        P("tp", "fs"),
        P(),
        P("tp", "fs"),
        P("tp", "fs"),
        P(),
        P(),
        P(),
        P(),
        P(),
        P(),
    )
    out_specs = P("fs", "tp")
    across = mesh.shape["tp"] // CORES
    if across == 2 and mesh.shape["fs"] % 2 == 0 and mesh.shape["fs"] > 2:
        depth = mesh.shape["fs"] // 2
        fine = Mesh(mesh.devices.reshape(depth, 2, 2, CORES), ("z", "y", "x", "c"))
        names = {"fs": ("z", "y"), "tp": ("x", "c")}

        def split(spec):
            return P(*(names.get(name) for name in spec))

        return jax.shard_map(
            functools.partial(column_plan, depth),
            mesh=fine,
            in_specs=tuple(split(spec) for spec in in_specs),
            out_specs=split(out_specs),
            check_vma=False,
        )
    return jax.shard_map(shards, mesh=mesh, in_specs=in_specs, out_specs=out_specs, check_vma=False)
```

```python
import functools

import jax
import jax.numpy as jnp
from jax import lax
from jax.experimental import pallas as pl
from jax.experimental.pallas import tpu as pltpu
from jax.sharding import Mesh
from jax.sharding import PartitionSpec as P

TAPS = 3
LENGTH = 128
CORES = 2

RESIDUAL_SCALE = 1.4142135623730951
HALF_STEP = 0.5
EPSILON = 1e-05
BY_AXIS = pl.DeviceIdType.MESH
ANY = pl.BlockSpec(memory_space=pl.ANY)
VMEM = pl.BlockSpec(memory_space=pltpu.VMEM)


def greet(depth, axes, others=()):
    barrier = pltpu.get_barrier_semaphore()
    z = lax.axis_index("z")
    targets = [{"z": lax.rem(z + d, depth)} for d in range(1, depth)]
    targets += [{axis: 1 - lax.axis_index(axis)} for axis in axes]
    targets += others
    for target in targets:
        pl.semaphore_signal(barrier, inc=1, device_id=target, device_id_type=BY_AXIS)
    pl.semaphore_wait(barrier, len(targets))


def remote(src, dst, send, recv, target):
    return pltpu.make_async_remote_copy(
        src_ref=src, dst_ref=dst, send_sem=send, recv_sem=recv, device_id=target, device_id_type=BY_AXIS
    )


def block_place(ref, px, pz, py, width):
    start = pl.multiple_of((pz * 2 + py) * width, width)
    return ref.at[:, px, :, pl.ds(start, width)]


def weights_kernel(
    depth, w_ref, m_ref, s_ref, t_ref, g_ref, held_ref, sa_ref, ta_ref,
    zsend, zrecv, ysend, yrecv, xsend, xrecv, dsend, drecv, msend, mrecv,
    ssend, srecv, tzsend, tzrecv, tcsend, tcrecv, local,
):
    z, y, x, c = (lax.axis_index(axis) for axis in ("z", "y", "x", "c"))
    width = w_ref.shape[-1]
    greet(depth, ("y", "x", "c"))

    mats = w_ref.shape[1]

    def place(px, pz, py, piece=slice(None)):
        start = pl.multiple_of((pz * 2 + py) * width, width)
        return g_ref.at[piece, px, :, pl.ds(start, width)]

    to_x, to_y, to_c = {"x": 1 - x}, {"y": 1 - y}, {"c": 1 - c}
    scale_sends, token_sends, z_copies, m_copies = [], [], [], []
    keeps = [
        pltpu.make_async_copy(s_ref, sa_ref.at[c, x, y, z], local.at[0]),
        pltpu.make_async_copy(t_ref, ta_ref.at[0, c], local.at[1]),
        pltpu.make_async_copy(w_ref.at[z], place(x, z, y), local.at[2]),
        pltpu.make_async_copy(m_ref.at[z], held_ref.at[0], local.at[3]),
    ]
    for copy in keeps:
        copy.start()
    beside = [remote(t_ref, ta_ref.at[0, c], tcsend.at[0], tcrecv.at[0], to_c)]
    beside[0].start()
    y_copies, x_copies, d_copies = [], [], []
    for p in range(mats):
        y_copies.append(remote(w_ref.at[z, p], place(x, z, y, p), ysend.at[p], yrecv.at[p], to_y))
        x_copies.append(remote(w_ref.at[z, p], place(x, z, y, p), xsend.at[p], xrecv.at[p], to_x))
        y_copies[p].start()
        x_copies[p].start()
    for d in range(1, depth):
        target = {"z": lax.rem(z + d, depth)}
        scale_sends.append(remote(s_ref, sa_ref.at[c, x, y, z], ssend.at[d], srecv.at[d], target))
        scale_sends[-1].start()
    for d in range(1, depth):
        target = lax.rem(z + d, depth)
        for p in range(mats):
            slot = d * mats + p
            z_copies.append(
                remote(w_ref.at[target, p], place(x, z, y, p), zsend.at[slot], zrecv.at[slot], {"z": target})
            )
            z_copies[-1].start()
    for d in range(1, depth):
        target = {"z": lax.rem(z + d, depth)}
        token_sends.append(remote(t_ref, ta_ref.at[d, c], tzsend.at[d], tzrecv.at[d], target))
        token_sends[-1].start()
    for d in range(1, depth):
        target = lax.rem(z + d, depth)
        m_copies.append(remote(m_ref.at[target], held_ref.at[d], msend.at[d], mrecv.at[d], {"z": target}))
        m_copies[-1].start()

    def relay(e):
        d, p = divmod(e, mats)
        source = lax.rem(z - d + depth, depth)
        if e % 2 == 0:
            y_copies[e].wait_recv()
            block = place(x, source, 1 - y, p)
            copy = remote(block, block, dsend.at[e], drecv.at[e], to_x)
        else:
            x_copies[e].wait_recv()
            block = place(1 - x, source, y, p)
            copy = remote(block, block, dsend.at[e], drecv.at[e], to_y)
        copy.start()
        d_copies.append(copy)

    keeps[0].wait()
    for copy in scale_sends:
        copy.wait()
    hops = (sa_ref.at[c, x, y], sa_ref.at[c, x], sa_ref.at[c])
    for k, (part, target) in enumerate(zip(hops, (to_y, to_x, to_c))):
        slot = (0, depth, depth + 1)[k]
        hop = remote(part, part, ssend.at[slot], srecv.at[slot], target)
        hop.start()
        hop.wait()
    count = depth * mats
    for e in range(mats, count):
        d, p = divmod(e, mats)
        block = place(x, lax.rem(z - d + depth, depth), y, p)
        z_copies[e - mats].wait_recv()
        ycopy = remote(block, block, ysend.at[e], yrecv.at[e], to_y)
        xcopy = remote(block, block, xsend.at[e], xrecv.at[e], to_x)
        ycopy.start()
        xcopy.start()
        y_copies.append(ycopy)
        x_copies.append(xcopy)
        relay(e - mats)
    for e in range(count - mats, count):
        relay(e)
    for d in range(1, depth):
        token_sends[d - 1].wait_recv()
        copy = remote(ta_ref.at[d, c], ta_ref.at[d, c], tcsend.at[d], tcrecv.at[d], to_c)
        copy.start()
        beside.append(copy)
    for e in range(count):
        (x_copies if e % 2 == 0 else y_copies)[e].wait_recv()
        d_copies[e].wait()
        y_copies[e].wait_send()
        x_copies[e].wait_send()
    for copy in beside:
        copy.wait()
    for copy in m_copies:
        copy.wait()
    for copy in z_copies + token_sends:
        copy.wait_send()
    for copy in keeps[1:]:
        copy.wait()


def spread_weights(depth, blocks, mixer_blocks, scale_block, own_rows):
    mats, rows, width = blocks.shape[1:]
    dma = pltpu.SemaphoreType.DMA
    return pl.pallas_call(
        functools.partial(weights_kernel, depth),
        out_shape=(
            jax.ShapeDtypeStruct((mats, 2, rows, depth * 2 * width), jnp.bfloat16),
            jax.ShapeDtypeStruct(mixer_blocks.shape, jnp.bfloat16),
            jax.ShapeDtypeStruct((CORES, 2, 2, depth) + scale_block.shape, jnp.float32),
            jax.ShapeDtypeStruct((depth, CORES) + own_rows.shape, jnp.bfloat16),
        ),
        in_specs=[ANY] * 4,
        out_specs=(ANY,) * 4,
        scratch_shapes=[dma((depth * mats,)) for _ in range(8)]
        + [dma((depth,)), dma((depth,))]
        + [dma((depth + 2,)), dma((depth + 2,))]
        + [dma((depth,)) for _ in range(4)]
        + [dma((4,))],
        compiler_params=pltpu.CompilerParams(collective_id=0, has_side_effects=True),
        name="spread_weights",
    )(blocks, mixer_blocks, scale_block, own_rows)


def dot_last(left, right):
    return lax.dot_general(left, right, (((1,), (1,)), ((), ())), preferred_element_type=jnp.float32)


def merged(ref, k):
    two, rows, features = ref.shape[1:]
    return ref[k].reshape(two * rows, features)


def feed_chunk(inputs, weights, factors, taps):
    gate_sum = dot_last(inputs, merged(weights, 0)) * factors[0:1]
    up_sum = dot_last(inputs, merged(weights, 1)) * factors[1:2]
    hidden = (gate_sum / (1.0 + jnp.exp(-gate_sum)) * up_sum).astype(jnp.bfloat16)
    return jnp.dot(hidden, merged(weights, 2), preferred_element_type=jnp.float32)


def mixer_chunk(inputs, weights, factors, taps):
    outgate = dot_last(inputs, merged(weights, 0)) * factors[0:1]
    ingate = dot_last(inputs, merged(weights, 1)) * factors[1:2]
    values = dot_last(inputs, merged(weights, 2)) * factors[2:3]
    mixed = ingate * values
    position = lax.rem(lax.broadcasted_iota(jnp.int32, mixed.shape, 0), LENGTH)
    convolved = taps[TAPS - 1 : TAPS] * mixed
    for back in range(1, TAPS):
        earlier = jnp.where(position >= back, pltpu.roll(mixed, back, 0), 0.0)
        convolved = convolved + taps[TAPS - 1 - back : TAPS - back] * earlier
    gated = (outgate * convolved).astype(jnp.bfloat16)
    return jnp.dot(gated, merged(weights, 3), preferred_element_type=jnp.float32)


def stage_kernel(depth, chunk, first, final, *refs):
    refs = list(refs)
    take = lambda n: [refs.pop(0) for _ in range(n)]
    w_ref, f_ref, k_ref, own_ref, scale_ref, gain_ref, shift_ref = take(7)
    if first:
        whole, held_ref = take(2)
        out_ref, m_ref = take(2)
    else:
        (out_ref,) = take(1)
    part, half, sums, got, hsend, hrecv, rsend, rrecv = take(8)
    z, c = lax.axis_index("z"), lax.axis_index("c")
    to_c = {"c": 1 - c}
    if first:
        ysend, yrecv, xsend, xrecv, dsend, drecv, local = take(7)
        y, x = lax.axis_index("y"), lax.axis_index("x")
        greet(depth, ("y", "x", "c"))
        width = held_ref.shape[-1]
        y_copies, x_copies, d_copies, keeps = [], [], [], []
        for d in range(depth):
            block = block_place(m_ref, x, lax.rem(z - d + depth, depth), y, width)
            y_copies.append(remote(held_ref.at[d], block, ysend.at[d], yrecv.at[d], {"y": 1 - y}))
            x_copies.append(remote(held_ref.at[d], block, xsend.at[d], xrecv.at[d], {"x": 1 - x}))
            keeps.append(pltpu.make_async_copy(held_ref.at[d], block, local.at[d]))
            y_copies[d].start()
            x_copies[d].start()
            keeps[d].start()
    else:
        whole, zsend, zrecv, csend, crecv = take(5)
        if final:
            sheet, fsend, frecv = take(3)
            x = lax.axis_index("x")
            greet(depth, ("x", "c"), [{"x": 1 - x, "c": 1 - c}])
        else:
            greet(depth, ("c",))
        beside = remote(own_ref, whole.at[0, c], csend.at[0], crecv.at[0], to_c)
        beside.start()
        across = []
        for d in range(1, depth):
            target = {"z": lax.rem(z + d, depth)}
            across.append(remote(own_ref, whole.at[d, c], zsend.at[d], zrecv.at[d], target))
            across[-1].start()
        whole[0, c] = own_ref[...]

    def share(d):
        target = {"z": lax.rem(z - d + depth, depth)}
        return remote(sums.at[d], got.at[d], rsend.at[d], rrecv.at[d], target)

    def handover(d):
        return remote(part.at[d, 1 - c], half.at[d], hsend.at[d], hrecv.at[d], to_c)

    def forward(d):
        return remote(whole.at[d, c], whole.at[d, c], csend.at[d], crecv.at[d], to_c)

    def step(i, carry):
        d = lax.rem(i + 1, depth) if first else i
        if not first:

            @pl.when(d > 0)
            def _():
                remote(own_ref, whole.at[d, c], zsend.at[d], zrecv.at[d], {"z": z}).wait_recv()
                forward(d).start()

            forward(d).wait_recv()
        rows = own_ref.shape[0]
        inputs = whole[d].reshape(CORES * rows, -1)
        total = chunk(inputs, w_ref, f_ref[...], k_ref[...])
        part[d] = total.astype(jnp.bfloat16).reshape(part.shape[1:])
        handover(d).start()
        handover(d).wait_recv()

        @pl.when(d > 0)
        def _():
            both = part[d, c].astype(jnp.float32) + half[d].astype(jnp.float32)
            sums[d] = both.astype(jnp.bfloat16)
            share(d).start()

        return carry

    lax.fori_loop(0, depth, step, 0)
    if first:
        for d in range(depth):
            source = lax.rem(z - d + depth, depth)
            if d % 2 == 0:
                y_copies[d].wait_recv()
                block = block_place(m_ref, x, source, 1 - y, width)
                copy = remote(block, block, dsend.at[d], drecv.at[d], {"x": 1 - x})
            else:
                x_copies[d].wait_recv()
                block = block_place(m_ref, 1 - x, source, y, width)
                copy = remote(block, block, dsend.at[d], drecv.at[d], {"y": 1 - y})
            copy.start()
            d_copies.append(copy)
    total = part[0, c].astype(jnp.float32) + half[0].astype(jnp.float32)
    for d in range(1, depth):
        share(d).wait_recv()
        total = total + got[d].astype(jnp.float32)
    summed = RESIDUAL_SCALE * own_ref[...].astype(jnp.float32) + total * scale_ref[...]
    count = summed.shape[1]
    average = jnp.sum(summed, -1, keepdims=True) / count
    mean_square = jnp.sum(summed * summed, -1, keepdims=True) / count
    variance = mean_square - average * average
    normed = (summed - average) * lax.rsqrt(variance + EPSILON) * gain_ref[...] + shift_ref[...]
    if final:
        rows, columns = own_ref.shape[0], out_ref.shape[1]
        own_place = x * CORES + c
        here = pl.ds(pl.multiple_of(own_place * rows, rows), rows)
        sheet[...] = normed.astype(jnp.bfloat16)
        leaving = []
        for k, (tx, tc) in enumerate(((1 - x, c), (1 - x, 1 - c), (x, 1 - c))):
            there = pl.ds(pl.multiple_of((tx * CORES + tc) * columns, columns), columns)
            leaving.append(
                remote(sheet.at[:, there], out_ref.at[here], fsend.at[k], frecv.at[k], {"x": tx, "c": tc})
            )
            leaving[-1].start()
        out_ref[here] = sheet[:, pl.ds(pl.multiple_of(own_place * columns, columns), columns)]
        for copy in leaving:
            copy.wait()
    else:
        out_ref[...] = normed.astype(jnp.bfloat16)
    for d in range(depth):
        handover(d).wait_send()
        if d > 0:
            share(d).wait_send()
    if first:
        for d in range(depth):
            (x_copies if d % 2 == 0 else y_copies)[d].wait_recv()
            for copy in (y_copies[d], x_copies[d]):
                copy.wait_send()
            d_copies[d].wait()
            keeps[d].wait()
    else:
        beside.wait_send()
        for d in range(1, depth):
            forward(d).wait_send()
            across[d - 1].wait_send()


def stage(depth, number, chunk, weights, factors, taps, own, scale, gain, shift, whole=None, held=None, final=False):
    rows, features = own.shape
    first = whole is not None
    dma = pltpu.SemaphoreType.DMA
    block = pltpu.VMEM((depth, rows, features), jnp.bfloat16)
    pair = pltpu.VMEM((depth, CORES, rows, features), jnp.bfloat16)
    operands = [weights, factors, taps, own, scale[None], gain[None], shift[None]]
    in_specs = [VMEM] * 7
    out_shape = [jax.ShapeDtypeStruct((rows, features), jnp.bfloat16)]
    out_specs = [VMEM]
    scratch = [pair, block, block, block] + [dma((depth,)) for _ in range(4)]
    if first:
        operands += [whole, held]
        in_specs += [VMEM, ANY]
        mats, part_rows, width = held.shape[1:]
        out_shape.append(jax.ShapeDtypeStruct((mats, 2, part_rows, depth * 2 * width), jnp.bfloat16))
        out_specs.append(ANY)
        scratch += [dma((depth,)) for _ in range(7)]
    else:
        scratch += [pair] + [dma((depth,)) for _ in range(4)]
    if final:
        out_shape = [jax.ShapeDtypeStruct((2 * CORES * rows, features // (2 * CORES)), jnp.bfloat16)]
        scratch += [pltpu.VMEM((rows, features), jnp.bfloat16), dma((3,)), dma((3,))]
    return pl.pallas_call(
        functools.partial(stage_kernel, depth, chunk, first, final),
        out_shape=tuple(out_shape),
        in_specs=in_specs,
        out_specs=tuple(out_specs),
        scratch_shapes=scratch,
        compiler_params=pltpu.CompilerParams(
            collective_id=number, has_side_effects=True, vmem_limit_bytes=40 * 1024 * 1024
        ),
        name=f"stage_{number}",
    )(*operands)


def column_plan(
    depth, tokens, gate_weight, up_weight, down_weight, gate_scale, up_scale, down_scale,
    bgate_weight, cgate_weight, value_weight, bgate_scale, cgate_scale, value_scale, conv_taps,
    mixout_weight, mixout_scale, first_gain, first_shift, mixer_gain, mixer_shift, last_gain, last_shift,
):
    z, c = lax.axis_index("z"), lax.axis_index("c")
    own = lax.all_to_all(tokens, ("x", "c"), 0, 1, tiled=True)

    def cut(matrix):
        return matrix.astype(jnp.bfloat16).reshape(depth, -1, matrix.shape[1])

    blocks = jnp.stack([cut(gate_weight.T), cut(up_weight.T), cut(down_weight)], axis=1)
    mixer_blocks = jnp.stack(
        [cut(m.T) for m in (bgate_weight, cgate_weight, value_weight)] + [cut(mixout_weight)], axis=1
    )
    channels = bgate_weight.shape[1] // depth
    pieces = (gate_scale, up_scale, down_scale, bgate_scale, cgate_scale, value_scale, mixout_scale)
    flat = jnp.concatenate([piece.reshape(-1) for piece in pieces])
    flat = jnp.pad(flat, (0, -flat.shape[0] % 1024)).reshape(-1, 128)
    feed_weights, held, scales, whole = spread_weights(depth, blocks, mixer_blocks, flat, own)
    scales = scales.reshape(scales.shape[:4] + (-1,))
    mine = lax.dynamic_index_in_dim(lax.dynamic_index_in_dim(scales, c, 0, False), z, 2, False)
    edges = [0]
    for piece in pieces:
        edges.append(edges[-1] + piece.shape[1])

    def unit_scale(k):
        return mine[:, :, edges[k] : edges[k + 1]].reshape(-1)

    def feature_scale(k):
        return scales[..., edges[k] : edges[k + 1]].transpose(1, 0, 3, 2, 4).reshape(-1)

    feed_factors = jnp.stack([unit_scale(0), unit_scale(1)])
    mixer_factors = jnp.stack([unit_scale(3), unit_scale(4), unit_scale(5)])
    down_cols, mixout_cols = HALF_STEP * feature_scale(2), feature_scale(6)
    taps = conv_taps.reshape(TAPS, 2, CORES, depth, channels)
    taps = lax.dynamic_index_in_dim(lax.dynamic_index_in_dim(taps, c, 2, False), z, 2, False)
    taps = taps.reshape(TAPS, -1)

    first, mixer_weights = stage(
        depth, 1, feed_chunk, feed_weights, feed_factors, taps, own, down_cols, first_gain, first_shift, whole, held
    )
    (second,) = stage(
        depth, 2, mixer_chunk, mixer_weights, mixer_factors, taps, first, mixout_cols, mixer_gain, mixer_shift
    )
    (last,) = stage(
        depth, 3, feed_chunk, feed_weights, feed_factors, taps, second, down_cols, last_gain, last_shift, final=True
    )
    return last


def add_rows(gathered, shard_piece):
    return jnp.dot(gathered, shard_piece, preferred_element_type=jnp.float32)


def features(inputs):
    return lax.all_gather(inputs, "tp", axis=1, tiled=True)


def post_norm(residual, branch, norm_gain, norm_shift):
    summed = RESIDUAL_SCALE * residual.astype(jnp.float32) + branch
    moments = lax.psum((jnp.sum(summed, -1), jnp.sum(summed * summed, -1)), "tp")
    feature_total = summed.shape[1] * lax.axis_size("tp")
    average = (moments[0] / feature_total)[:, None]
    mean_square = (moments[1] / feature_total)[:, None]
    variance = mean_square - average * average
    return ((summed - average) * lax.rsqrt(variance + EPSILON) * norm_gain + norm_shift).astype(
        jnp.bfloat16
    )


def spread_back(weight_cols, left_rows):
    return (
        lax.psum_scatter(
            lax.dot_general(
                weight_cols, left_rows, (((0,), (1,)), ((), ())), preferred_element_type=jnp.float32
            ).astype(jnp.bfloat16),
            "tp",
            scatter_dimension=0,
            tiled=True,
        )
        .astype(jnp.float32)
        .T
    )


def shards(
    tokens,
    gate_weight,
    up_weight,
    down_weight,
    gate_scale,
    up_scale,
    down_scale,
    bgate_weight,
    cgate_weight,
    value_weight,
    bgate_scale,
    cgate_scale,
    value_scale,
    conv_taps,
    mixout_weight,
    mixout_scale,
    first_gain,
    first_shift,
    mixer_gain,
    mixer_shift,
    last_gain,
    last_shift,
):
    scales = (
        lax.all_gather(gate_scale, "fs", axis=1, tiled=True),
        lax.all_gather(up_scale, "fs", axis=1, tiled=True),
        lax.all_gather(down_scale, "fs", axis=1, tiled=True),
        lax.all_gather(bgate_scale, "fs", axis=1, tiled=True),
        lax.all_gather(cgate_scale, "fs", axis=1, tiled=True),
        lax.all_gather(value_scale, "fs", axis=1, tiled=True),
        lax.all_gather(mixout_scale, "fs", axis=1, tiled=True),
    )
    gate_cols, up_cols, down_cols, bgate_cols, cgate_cols, value_cols, mixout_cols = [
        scale_row.reshape(-1) for scale_row in scales
    ]
    tp_index = lax.axis_index("tp")
    columns = tokens.shape[1]

    def own_part(vector):
        return lax.dynamic_slice_in_dim(vector, tp_index * columns, columns)

    gate_low = gate_weight.astype(jnp.bfloat16)
    up_low = up_weight.astype(jnp.bfloat16)
    down_low = down_weight.astype(jnp.bfloat16)
    kept_gate, kept_up = (
        lax.all_gather(gate_low, "fs", axis=0, tiled=True),
        lax.all_gather(up_low, "fs", axis=0, tiled=True),
    )
    kept_down = lax.all_gather(down_low, "fs", axis=1, tiled=True)

    def channel_mix(gathered):
        gate_sum = jnp.dot(gathered, kept_gate, preferred_element_type=jnp.float32)
        up_sum = jnp.dot(gathered, kept_up, preferred_element_type=jnp.float32)
        hidden = (jax.nn.silu(gate_sum * gate_cols) * (up_sum * up_cols)).astype(jnp.bfloat16)
        return HALF_STEP * (spread_back(kept_down, hidden) * down_cols)

    first = post_norm(
        tokens, channel_mix(features(tokens)), own_part(first_gain), own_part(first_shift)
    )
    gathered = features(first)
    bgate_low = bgate_weight.astype(jnp.bfloat16)
    channels = bgate_low.shape[1]
    outgate = add_rows(gathered, lax.all_gather(bgate_low, "fs", axis=0, tiled=True))
    ingate = add_rows(
        gathered, lax.all_gather(cgate_weight.astype(jnp.bfloat16), "fs", axis=0, tiled=True)
    )
    values = add_rows(
        gathered, lax.all_gather(value_weight.astype(jnp.bfloat16), "fs", axis=0, tiled=True)
    )
    tap_weights = lax.dynamic_slice_in_dim(conv_taps, tp_index * channels, channels, 1)
    mixed = (ingate * cgate_cols * (values * value_cols)).reshape(-1, LENGTH, channels)
    padded = jnp.pad(mixed, ((0, 0), (TAPS - 1, 0), (0, 0)))
    convolved = jnp.zeros(mixed.shape, jnp.float32)
    for tap_index in range(TAPS):
        convolved = convolved + tap_weights[tap_index] * padded[:, tap_index : tap_index + LENGTH]
    gated = (outgate * bgate_cols * convolved.reshape(-1, channels)).astype(jnp.bfloat16)
    mix_full = lax.all_gather(mixout_weight.astype(jnp.bfloat16), "fs", axis=1, tiled=True)
    second = post_norm(
        first,
        spread_back(mix_full, gated) * mixout_cols,
        own_part(mixer_gain),
        own_part(mixer_shift),
    )
    return post_norm(
        second, channel_mix(features(second)), own_part(last_gain), own_part(last_shift)
    )


def solution(mesh):
    in_specs = (
        P("fs", "tp"),
        P("fs", "tp"),
        P("fs", "tp"),
        P("tp", "fs"),
        P("tp", "fs"),
        P("tp", "fs"),
        P("tp", "fs"),
        P("fs", "tp"),
        P("fs", "tp"),
        P("fs", "tp"),
        P("tp", "fs"),
        P("tp", "fs"),
        P("tp", "fs"),
        P(),
        P("tp", "fs"),
        P("tp", "fs"),
        P(),
        P(),
        P(),
        P(),
        P(),
        P(),
    )
    out_specs = P("fs", "tp")
    across = mesh.shape["tp"] // CORES
    if across == 2 and mesh.shape["fs"] % 2 == 0 and mesh.shape["fs"] > 2:
        depth = mesh.shape["fs"] // 2
        fine = Mesh(mesh.devices.reshape(depth, 2, 2, CORES), ("z", "y", "x", "c"))
        names = {"fs": ("z", "y"), "tp": ("x", "c")}

        def split(spec):
            return P(*(names.get(name) for name in spec))

        return jax.shard_map(
            functools.partial(column_plan, depth),
            mesh=fine,
            in_specs=tuple(split(spec) for spec in in_specs),
            out_specs=split(out_specs),
            check_vma=False,
        )
    return jax.shard_map(shards, mesh=mesh, in_specs=in_specs, out_specs=out_specs, check_vma=False)
```
